32 devices in a mesh: sp: 8 (over z, y), tp: 4 (over x, core).
Axes of the slice: x: 2, y: 2, z: 4, core: 2. Of those that a mesh axis runs over, the one named last changes fastest.
Arguments:
- layer_input: bfloat16 [4096, 2048], P('sp'), may hold values from -6 to 6
- out_cot: bfloat16 [4096, 2048], P('sp'), may hold values from -6 to 6
- expert_ids: int32 [4096, 2], P('sp'), may hold values from 0 to 7, all different within a row; in each aligned block of 512 rows (0 to 511, 512 to 1023, ...) at most 160 rows name the same one
- route_weight: float32 [4096, 2], P('sp'), may hold values from 0.1 to 1
- w_gate: bfloat16 [8, 2048, 1024], P('sp', None, 'tp'), may hold values from -0.125 to 0.125
- w_up: bfloat16 [8, 2048, 1024], P('sp', None, 'tp'), may hold values from -0.125 to 0.125
- w_down: bfloat16 [8, 1024, 2048], P('sp', 'tp'), may hold values from -0.1875 to 0.1875
- out_proj: bfloat16 [2048, 1024], P(None, 'tp'), may hold values from -0.1875 to 0.1875
- rec_input: bfloat16 [4096, 1024], P('sp', 'tp'), may hold values from -6 to 6
- gate_input: bfloat16 [4096, 1024], P('sp', 'tp'), may hold values from -6 to 6
- prev_state: float32 [4096, 1024], P('sp', 'tp'), may hold values from -6 to 6
- decay_param: float32 [1024], replicated, may hold values from 4 to 20
- extra_decay: float32 [8, 4096], P('tp', 'sp'), may hold values from -3 to 0, as said below
- gate_a_w: bfloat16 [8, 128, 128], replicated, may hold values from -0.5 to 0.5
- gate_i_w: bfloat16 [8, 128, 128], replicated, may hold values from -0.5 to 0.5
Outputs:
- grad_gate: float32 [8, 2048, 1024], P('sp', None, 'tp')
- grad_up: float32 [8, 2048, 1024], P('sp', None, 'tp')
- grad_down: float32 [8, 1024, 2048], P('sp', 'tp')
- grad_out_proj: float32 [2048, 1024], P('sp', 'tp')
- rec_input_grad: bfloat16 [4096, 1024], P('sp', 'tp')
- gate_input_grad: bfloat16 [4096, 1024], P('sp', 'tp')
The draws below stay inside these ranges and needn't reach their ends.
Inputs may be any that keep to these rules, and one draw needn't show every extreme that they name: `expert_ids`: each row names 2 different experts; among the slots of the tokens of one sp index (aligned blocks of 512 rows) no expert is named more than 160 times, and in every draw some expert is named exactly 160 times in some block. `extra_decay`: every entry is at most -0.05 / 4096.
All inputs are finite; a program needn't handle non-finite values.
Results may differ from the reference program's by a relative error of at most 0.017.
Values may be sent and summed in bfloat16 or wider, within the bound.
A program may use at most 128 MiB of HBM per device.

```python
import math
import jax
import jax.numpy as jnp
import numpy as np
from jax import lax

D = 2048
FF = 1024
RECURRENT_HEADS = 8
HEAD_DIM = 128
TOP = 2
TOK_DEV = 512
D_LRU = 1024
EXPERTS = 8
TOKENS = 4096
CAP = 160
EXP_ROWS = 1280
N_SP = 8
N_TP = 4


def draw_decay_param(key, part):
    head_key, rate_random_key = jax.random.split(jax.random.fold_in(key, 11))
    picks = jax.random.randint(head_key, (RECURRENT_HEADS,), 0, 10)
    quick = picks < 5
    unit = jax.random.uniform(rate_random_key, (RECURRENT_HEADS, HEAD_DIM), jnp.float32)
    quick_rate = 0.0025 * 4.0 ** unit
    slow_rate = 0.02 / TOKENS * 5.0 ** unit
    rate = jnp.where(quick[:, None], quick_rate, slow_rate).reshape(RECURRENT_HEADS * HEAD_DIM)
    return (-jnp.log(jnp.expm1(rate))).astype(jnp.float32)


def draw_extra_decay(key, part):
    rate_random_key, spike_random_key, placement_random_key = jax.random.split(jax.random.fold_in(key, 23), 3)
    blocks = TOKENS // TOK_DEV
    unit = jax.random.uniform(rate_random_key, (RECURRENT_HEADS, blocks), jnp.float32)
    block_rate = 0.1 / TOKENS * 10.0 ** unit
    token_wise = jnp.repeat(block_rate, TOK_DEV, axis=1)
    spots = jax.random.randint(placement_random_key, (RECURRENT_HEADS, 3), 0, TOKENS)
    retained_mask = jax.random.uniform(spike_random_key, (RECURRENT_HEADS, 3), jnp.float32, 0.5, 0.8)
    match_count = (spots[:, :, None] == jnp.arange(TOKENS, dtype=jnp.int32)[None, None, :]).astype(jnp.float32)
    spike_amount = jnp.sum(match_count * jnp.log(retained_mask)[:, :, None], axis=1)
    return (spike_amount - token_wise).astype(jnp.float32)


def raised(values, stream_key, source, target, blocks, factor):
    def block_of(position):
        return (jnp.arange(values.shape[position]) // (values.shape[position] // blocks)).reshape((-1,) + (1,) * (values.ndim - 1 - position))

    one_side = jax.random.permutation(stream_key, blocks)[block_of(target)]
    far = (block_of(target) + blocks // 2) % blocks
    return jnp.where((block_of(source) == one_side) | (block_of(source) == far), factor * values, values)


def shard_levels(stream_key, shape, pieces, low, high):
    loudness = 1.0
    for axis_at, parts in pieces:
        steps = jax.random.uniform(jax.random.fold_in(jax.random.fold_in(stream_key, 6), axis_at), (parts,), jnp.float32, low / len(pieces), high / len(pieces))
        loudness = loudness * jnp.repeat(jnp.exp(steps), shape[axis_at] // parts).reshape((-1,) + (1,) * (len(shape) - 1 - axis_at))
    return loudness


def deal_out(stream_key, own, number, rows, amount, top, reach, skew):
    ranking = jax.random.permutation(stream_key, amount)
    crowded, usual = portions_of(amount, rows * top, reach, skew, True), portions_of(amount, rows * top, reach, skew, False)
    places = jnp.arange(amount)

    def named(lengths, turn):
        used = int((lengths > 0).sum())
        fixed = max(1, used // 4)
        shifted = fixed + (places - fixed + turn * (used - fixed)) % max(1, amount - fixed)
        return jnp.zeros((amount,), jnp.int32).at[ranking[jnp.where(places < fixed, places, shifted)]].set(jnp.asarray(lengths, jnp.int32))

    lengths = jnp.where(number % 4 == 0, named(crowded, number // 4), named(usual, number - number // 4 - 1))
    mixed = jax.random.permutation(jax.random.fold_in(own, 3), amount)
    giver, sink = mixed[0:amount // 2 * 2:2], mixed[1:amount // 2 * 2:2]
    room = jnp.minimum(lengths[giver] - 1, reach - lengths[sink]) // 2
    room = jnp.where((giver == ranking[0]) | (sink == ranking[0]) | (lengths[sink] == 0), 0, jnp.maximum(room, 0))
    shifted = jax.random.randint(jax.random.fold_in(own, 4), (amount // 2,), 0, 1 << 20) % (room + 1)
    lengths = lengths.at[giver].add(-shifted).at[sink].add(shifted)
    items = jnp.searchsorted(jnp.cumsum(lengths), jnp.arange(rows * top), side="right").astype(jnp.int32)
    table = items.reshape(top, rows).T
    table = table[jax.random.permutation(jax.random.fold_in(own, 1), rows)]
    turn = jax.random.randint(jax.random.fold_in(own, 2), (rows, 1), 0, top)
    return jnp.take_along_axis(table, (jnp.arange(top)[None, :] + turn) % top, axis=1)


def portions_of(amount, total, limit, lean, full):
    loads = [(1 << 20) // math.isqrt(grade ** lean) + 1 for grade in range(1, amount + 1)]
    largest = limit if full else min(limit, max(-(-total // amount), total * loads[0] // sum(loads)))
    least = 1 if total - largest >= amount - 1 else 0
    holding, rest = [largest] + [least] * (amount - 1), total - largest - least * (amount - 1)
    while rest > 0:
        candidates = [i for i in range(1, amount) if holding[i] < largest] or [i for i in range(1, amount) if holding[i] < limit]
        pool, left = sum([loads[i] for i in candidates]), rest
        for i in candidates:
            extra = min(limit - holding[i], max(1, left * loads[i] // pool), rest)
            holding[i] = holding[i] + extra
            rest = rest - extra
    return np.array(holding)


def centred(key, dims, width, limit, cuts=(), kind=jnp.bfloat16):
    entries = width * jax.random.normal(key, dims, jnp.float32)
    if cuts:
        entries = entries * shard_levels(key, dims, cuts, -0.22, 0.18)
    return jnp.clip(entries, -limit, limit).astype(kind)


def noise_with(rng, extent, width, most, cuts, heavy, kind=jnp.bfloat16):
    entries = width * jax.random.normal(rng, extent, jnp.float32)
    if cuts:
        entries = entries * shard_levels(rng, extent, cuts, -0.22, 0.18)
    return jnp.clip(raised(entries, jax.random.fold_in(rng, 3), *heavy), -most, most).astype(kind)


def setup_inputs(seed: int = 0) -> dict:
    seeds = jax.random.split(jax.random.key(seed), 16)
    layer_input = centred(seeds[0], (TOKENS, D), 1.0, 6.0, ((0, 8),))
    out_cot = noise_with(seeds[1], (TOKENS, D), 1.0, 6.0, ((0, 8),), (0, 1, 8, 2.0))
    expert_ids_keys = jax.random.split(jax.random.fold_in(seeds[2], 1), TOKENS // TOK_DEV)
    expert_ids_turns = jax.random.permutation(jax.random.fold_in(seeds[2], 3), TOKENS // TOK_DEV)
    expert_ids = jax.vmap(lambda own, number: deal_out(jax.random.fold_in(seeds[2], 2), own, number, TOK_DEV, EXPERTS, TOP, CAP, 1))(expert_ids_keys, expert_ids_turns).reshape((TOKENS, TOP))
    route_weight = jnp.clip(0.1 + 0.9 * jax.random.uniform(seeds[3], (TOKENS, TOP), jnp.float32) ** shard_levels(seeds[3], (TOKENS, TOP), ((0, 8),), -0.2, 0.2), 0.1, 1.0)
    w_gate = centred(seeds[4], (EXPERTS, D, FF), D ** -0.5, 0.125, ((0, 8), (2, 4)))
    w_up = centred(seeds[5], (EXPERTS, D, FF), D ** -0.5, 0.125, ((0, 8), (2, 4)))
    w_down = centred(seeds[6], (EXPERTS, FF, D), FF ** -0.5, 0.1875, ((0, 8), (1, 4)))
    out_proj = centred(seeds[7], (D, D_LRU), D_LRU ** -0.5, 0.1875, ((1, 4),))
    rec_input = centred(seeds[8], (TOKENS, D_LRU), 1.0, 6.0, ((0, 8), (1, 4)))
    gate_input = centred(seeds[9], (TOKENS, D_LRU), 1.0, 6.0, ((0, 8), (1, 4)))
    prev_state = centred(seeds[10], (TOKENS, D_LRU), 1.0, 6.0, ((0, 8), (1, 4)), jnp.float32)
    decay_param = draw_decay_param(jax.random.fold_in(seeds[15], 71), 0)
    extra_decay = draw_extra_decay(jax.random.fold_in(seeds[15], 71), 0)
    gate_a_w = centred(seeds[13], (RECURRENT_HEADS, HEAD_DIM, HEAD_DIM), HEAD_DIM ** -0.5, 0.5)
    gate_i_w = centred(seeds[14], (RECURRENT_HEADS, HEAD_DIM, HEAD_DIM), HEAD_DIM ** -0.5, 0.5)
    return {"layer_input": layer_input, "out_cot": out_cot, "expert_ids": expert_ids, "route_weight": route_weight, "w_gate": w_gate, "w_up": w_up, "w_down": w_down, "out_proj": out_proj, "rec_input": rec_input, "gate_input": gate_input, "prev_state": prev_state, "decay_param": decay_param, "extra_decay": extra_decay, "gate_a_w": gate_a_w, "gate_i_w": gate_i_w}


gelu_scale = 0.7978845608028654
gelu_cubic = 0.044715
decay_factor = 8.0

def gelu_pair(values_in):
    inner = gelu_scale * (values_in + gelu_cubic * values_in * values_in * values_in)
    bend = jnp.tanh(inner)
    active = 0.5 * values_in * (1.0 + bend)
    slope = 0.5 * (1.0 + bend) + 0.5 * values_in * (1.0 - bend * bend) * gelu_scale * (1.0 + 3.0 * gelu_cubic * values_in * values_in)
    return (active, slope)

def head_product(row_block, weights, backward):
    blocks = row_block.astype(jnp.float32).reshape(row_block.shape[0], RECURRENT_HEADS, HEAD_DIM)
    wide = weights.astype(jnp.float32)
    if backward:
        result = jnp.einsum('nhe,hde->nhd', blocks, wide)
    else:
        result = jnp.einsum('nhd,hde->nhe', blocks, wide)
    return result.reshape(row_block.shape[0], RECURRENT_HEADS * HEAD_DIM)

def chain_link(earlier, later):
    return (earlier[0] * later[0], later[0] * earlier[1] + later[1])

def expert_backward(operands):
    row_block, cot_block, gate_w, up_w, down_w = operands
    gate_pre = jnp.dot(row_block, gate_w, preferred_element_type=jnp.float32)
    up_pre = jnp.dot(row_block, up_w, preferred_element_type=jnp.float32)
    sigma = jax.nn.sigmoid(gate_pre)
    swish = gate_pre * sigma
    hidden = (swish * up_pre).astype(jnp.bfloat16)
    hidden_cot = jnp.dot(cot_block, down_w.T, preferred_element_type=jnp.float32)
    grad_down = jnp.dot(hidden.T, cot_block, preferred_element_type=jnp.float32)
    gate_cot = (hidden_cot * up_pre * sigma * (1.0 + gate_pre * (1.0 - sigma))).astype(jnp.bfloat16)
    up_cot = (hidden_cot * swish).astype(jnp.bfloat16)
    grad_gate = jnp.dot(row_block.T, gate_cot, preferred_element_type=jnp.float32)
    grad_up = jnp.dot(row_block.T, up_cot, preferred_element_type=jnp.float32)
    part_width = FF // N_TP
    gate_groups = gate_cot.astype(jnp.float32).reshape(EXP_ROWS, N_TP, part_width)
    up_groups = up_cot.astype(jnp.float32).reshape(EXP_ROWS, N_TP, part_width)
    gate_wide = gate_w.astype(jnp.float32).reshape(D, N_TP, part_width)
    up_wide = up_w.astype(jnp.float32).reshape(D, N_TP, part_width)
    terms = jnp.einsum('rgf,dgf->grd', gate_groups, gate_wide) + jnp.einsum('rgf,dgf->grd', up_groups, up_wide)
    rounded = lax.optimization_barrier(terms.astype(jnp.bfloat16))
    row_cot = lax.optimization_barrier(jnp.sum(rounded.astype(jnp.float32), axis=0)).astype(jnp.bfloat16)
    return (grad_gate, grad_up, grad_down, row_cot)

def reference(layer_input, out_cot, expert_ids, route_weight, w_gate, w_up, w_down, out_proj, rec_input, gate_input, prev_state, decay_param, extra_decay, gate_a_w, gate_i_w):
    slot_total = TOKENS * TOP
    device_ids = expert_ids.reshape(N_SP, TOK_DEV * TOP)
    onehot = (device_ids[:, :, None] == jnp.arange(EXPERTS, dtype=jnp.int32)[None, None, :]).astype(jnp.int32)
    earlier_count = lax.optimization_barrier(jnp.sum((jnp.cumsum(onehot, axis=1) - onehot) * onehot, axis=2)).astype(jnp.int32)
    source_index = jnp.arange(N_SP, dtype=jnp.int32)[:, None]
    places = (source_index * CAP + earlier_count).reshape(slot_total).astype(jnp.int32)
    flat_ids = expert_ids.reshape(slot_total).astype(jnp.int32)
    token_index = jnp.arange(slot_total, dtype=jnp.int32) // TOP
    weighted = (route_weight[:, :, None] * out_cot[:, None, :].astype(jnp.float32)).astype(jnp.bfloat16).reshape(slot_total, D)
    row_buffer = jnp.zeros((EXPERTS, EXP_ROWS, D), jnp.bfloat16).at[flat_ids, places].set(layer_input[token_index])
    cot_buffer = jnp.zeros((EXPERTS, EXP_ROWS, D), jnp.bfloat16).at[flat_ids, places].set(weighted)
    grad_gate, grad_up, grad_down, back_buffer = lax.map(expert_backward, (row_buffer, cot_buffer, w_gate, w_up, w_down))
    slot_cot = back_buffer[flat_ids, places].astype(jnp.float32).reshape(TOKENS, TOP, D)
    layer_cot = (out_cot.astype(jnp.float32) + lax.optimization_barrier(jnp.sum(slot_cot, axis=1))).astype(jnp.bfloat16)
    mix_cot = jnp.dot(layer_cot, out_proj, preferred_element_type=jnp.float32)
    rgate = jax.nn.sigmoid(head_product(rec_input, gate_a_w, False))
    igate = jax.nn.sigmoid(head_product(rec_input, gate_i_w, False))
    rate_scale = decay_factor * jax.nn.softplus(-decay_param)
    log_decay = -rate_scale[None, :] * rgate + jnp.repeat(extra_decay.T, HEAD_DIM, axis=1)
    decay = jnp.exp(log_decay)
    scale = jnp.sqrt(-jnp.expm1(2.0 * log_decay))
    values_in = rec_input.astype(jnp.float32)
    state = decay * prev_state + scale * igate * values_in
    gate_act, gate_slope = gelu_pair(gate_input.astype(jnp.float32))
    rec_output = (state * gate_act).astype(jnp.bfloat16)
    grad_out_proj = jnp.dot(layer_cot.T, rec_output, preferred_element_type=jnp.float32)
    next_decay = jnp.concatenate([decay[1:], jnp.zeros((1, D_LRU), jnp.float32)], axis=0)
    drive = mix_cot * gate_act
    _, state_cot = lax.associative_scan(chain_link, (next_decay, drive), reverse=True)
    gate_input_grad = (mix_cot * state * gate_slope).astype(jnp.bfloat16)
    log_cot = state_cot * (decay * prev_state - decay * decay / scale * igate * values_in)
    a_pre_cot = (log_cot * -rate_scale[None, :] * rgate * (1.0 - rgate)).astype(jnp.bfloat16)
    i_pre_cot = (state_cot * scale * values_in * igate * (1.0 - igate)).astype(jnp.bfloat16)
    rec_input_grad = (state_cot * scale * igate + head_product(a_pre_cot, gate_a_w, True) + head_product(i_pre_cot, gate_i_w, True)).astype(jnp.bfloat16)
    return (grad_gate, grad_up, grad_down, grad_out_proj, rec_input_grad, gate_input_grad)
```

```python
import functools

import jax
import jax.numpy as jnp
from jax import lax
from jax.experimental import pallas as pl
from jax.experimental.pallas import tpu as pltpu
from jax.sharding import PartitionSpec as P

gelu_scale = 0.7978845608028654
gelu_cubic = 0.044715
decay_factor = 8.0


def exchange_kernel(kinds, axis, *refs):
    pairs = len(kinds)
    sources, targets = refs[:pairs], refs[pairs : 2 * pairs]
    send_sem, recv_sem, local_sem = refs[2 * pairs :]
    count = targets[0].shape[0]
    place = lax.axis_index(axis)
    barrier = pltpu.get_barrier_semaphore()
    for step in range(1, count):
        pl.semaphore_signal(
            barrier,
            inc=1,
            device_id={axis: lax.rem(place + step, count)},
            device_id_type=pl.DeviceIdType.MESH,
        )
    pl.semaphore_wait(barrier, count - 1)
    copies = []
    for which in range(pairs):
        for step in range(1, count):
            peer = lax.rem(place + step, count)
            source = sources[which].at[peer] if kinds[which] else sources[which]
            copy = pltpu.make_async_remote_copy(
                src_ref=source,
                dst_ref=targets[which].at[place],
                send_sem=send_sem.at[which, step],
                recv_sem=recv_sem.at[which, step],
                device_id={axis: peer},
                device_id_type=pl.DeviceIdType.MESH,
            )
            copy.start()
            copies.append(copy)
    for which in range(pairs):
        source = sources[which].at[place] if kinds[which] else sources[which]
        copy = pltpu.make_async_copy(source, targets[which].at[place], local_sem.at[which])
        copy.start()
        copies.append(copy)
    for copy in copies:
        copy.wait()


def exchange(arrays, kinds, axis, number):
    count = lax.axis_size(axis)
    shapes = [
        jax.ShapeDtypeStruct(a.shape if kind else (count,) + a.shape, a.dtype)
        for a, kind in zip(arrays, kinds)
    ]
    spec = pl.BlockSpec(memory_space=pltpu.VMEM)
    return pl.pallas_call(
        functools.partial(exchange_kernel, kinds, axis),
        in_specs=[spec] * len(arrays),
        out_specs=[spec] * len(arrays),
        out_shape=shapes,
        scratch_shapes=[
            pltpu.SemaphoreType.DMA((len(arrays), count)),
            pltpu.SemaphoreType.DMA((len(arrays), count)),
            pltpu.SemaphoreType.DMA((len(arrays),)),
        ],
        compiler_params=pltpu.CompilerParams(collective_id=number, has_side_effects=True),
        cost_estimate=pl.CostEstimate(
            flops=0, bytes_accessed=40 * arrays[0].size, transcendentals=0
        ),
    )(*arrays)


def carried_in(gathered, axis):
    count = lax.axis_size(axis)
    place = lax.axis_index(axis)
    carry = jnp.zeros_like(gathered[0, 0])
    for source in range(count - 1, 0, -1):
        step = gathered[source, 1] + gathered[source, 0] * carry
        carry = jnp.where(source > place, step, carry)
    return carry


def scan_kernel(link_ref, drive_ref, product_ref, total_ref):
    link = link_ref[...]
    total = drive_ref[...]
    rows, cols = link.shape
    row_index = lax.broadcasted_iota(jnp.int32, (rows, cols), 0)
    step = 1
    while step < rows:
        if step < 8:
            inside = row_index < rows - step
            later_link = jnp.where(inside, pltpu.roll(link, rows - step, 0), 1.0)
            later_total = jnp.where(inside, pltpu.roll(total, rows - step, 0), 0.0)
        else:
            later_link = jnp.concatenate([link[step:], jnp.ones((step, cols), jnp.float32)], axis=0)
            later_total = jnp.concatenate(
                [total[step:], jnp.zeros((step, cols), jnp.float32)], axis=0
            )
        total = total + link * later_total
        link = link * later_link
        step *= 2
    product_ref[...] = link
    total_ref[...] = total


def reverse_scan(link, drive):
    rows, cols = link.shape
    lanes = 128
    spec = pl.BlockSpec((rows, lanes), lambda i: (0, i))
    return pl.pallas_call(
        scan_kernel,
        grid=(cols // lanes,),
        in_specs=[spec, spec],
        out_specs=[spec, spec],
        out_shape=[jax.ShapeDtypeStruct((rows, cols), jnp.float32)] * 2,
        cost_estimate=pl.CostEstimate(
            flops=40 * rows * cols, bytes_accessed=16 * rows * cols, transcendentals=0
        ),
    )(link, drive)


def gelu_pair(values_in):
    inner = gelu_scale * (values_in + gelu_cubic * values_in * values_in * values_in)
    bend = jnp.tanh(inner)
    active = 0.5 * values_in * (1.0 + bend)
    slope = 0.5 * (1.0 + bend) + 0.5 * values_in * (1.0 - bend * bend) * gelu_scale * (
        1.0 + 3.0 * gelu_cubic * values_in * values_in
    )
    return (active, slope)


def head_product(row_block, weights, backward):
    heads = weights.shape[0]
    head_width = weights.shape[1]
    blocks = row_block.reshape(row_block.shape[0], heads, head_width)
    if backward:
        result = jnp.einsum("nhe,hde->nhd", blocks, weights, preferred_element_type=jnp.float32)
    else:
        result = jnp.einsum("nhd,hde->nhe", blocks, weights, preferred_element_type=jnp.float32)
    return result.reshape(row_block.shape[0], heads * head_width)


def slot_places(expert_ids, expert_count, capacity):
    flat_ids = expert_ids.reshape(-1)
    onehot = (flat_ids[:, None] == jnp.arange(expert_count, dtype=jnp.int32)[None, :]).astype(
        jnp.int32
    )
    earlier_count = jnp.sum((jnp.cumsum(onehot, axis=0) - onehot) * onehot, axis=1)
    return flat_ids * capacity + earlier_count


def per_device(
    layer_input,
    out_cot,
    expert_ids,
    route_weight,
    w_gate,
    w_up,
    w_down,
    out_proj,
    rec_input,
    gate_input,
    prev_state,
    decay_param,
    extra_decay,
    gate_a_w,
    gate_i_w,
):
    sources = lax.axis_size("sp")
    local_experts = w_gate.shape[0]
    expert_count = local_experts * sources
    tok_rows, width = layer_input.shape
    top_count = expert_ids.shape[1]
    capacity = 5 * tok_rows * top_count // (4 * expert_count)
    slot_count = tok_rows * top_count
    places = slot_places(expert_ids, expert_count, capacity)
    buffer_rows = expert_count * capacity
    token_places = places.reshape(tok_rows, top_count)
    row_index = jnp.arange(buffer_rows, dtype=jnp.int32)
    hits = row_index[:, None, None] == token_places.T[None, :, :]
    pick = jnp.any(hits, axis=1).astype(jnp.bfloat16)
    row_weight = jnp.sum(jnp.where(hits, route_weight.T[None, :, :], 0.0), axis=(1, 2))
    members = lax.axis_size("tp")
    piece = width // members
    first_col = lax.rem(lax.axis_index("tp"), members) * piece

    def deliver(array, weight, number):
        cols = lax.dynamic_slice_in_dim(array, first_col, piece, 1)
        rows = jnp.dot(pick, cols, preferred_element_type=jnp.float32)
        if weight is not None:
            rows = rows * weight[:, None]
        blocks = rows.astype(jnp.bfloat16).reshape(sources, buffer_rows // sources, piece)
        got = exchange([blocks], [True], "sp", number)[0].reshape(buffer_rows, piece)
        return lax.all_gather(got, "tp", axis=1, tiled=True)

    got_rows = deliver(layer_input, None, 0)
    got_cot = deliver(out_cot, row_weight, 1)

    def by_expert(array):
        col_count = array.shape[-1]
        return jnp.swapaxes(
            array.reshape(sources, local_experts, capacity, col_count), 0, 1
        ).reshape(local_experts, sources * capacity, col_count)

    expert_rows = by_expert(got_rows)
    expert_cot = by_expert(got_cot)
    gate_pre = jnp.einsum("erd,edf->erf", expert_rows, w_gate, preferred_element_type=jnp.float32)
    up_pre = jnp.einsum("erd,edf->erf", expert_rows, w_up, preferred_element_type=jnp.float32)
    sigma = jax.nn.sigmoid(gate_pre)
    swish = gate_pre * sigma
    hidden = (swish * up_pre).astype(jnp.bfloat16)
    hidden_cot = jnp.einsum("erd,efd->erf", expert_cot, w_down, preferred_element_type=jnp.float32)
    grad_down = jnp.einsum("erf,erd->efd", hidden, expert_cot, preferred_element_type=jnp.float32)
    gate_cot = (hidden_cot * up_pre * sigma * (1.0 + gate_pre * (1.0 - sigma))).astype(jnp.bfloat16)
    up_cot = (hidden_cot * swish).astype(jnp.bfloat16)
    grad_gate = jnp.einsum(
        "erd,erf->edf", expert_rows, gate_cot, preferred_element_type=jnp.float32
    )
    grad_up = jnp.einsum("erd,erf->edf", expert_rows, up_cot, preferred_element_type=jnp.float32)
    partial_value = jnp.einsum(
        "erf,edf->erd", gate_cot, w_gate, preferred_element_type=jnp.float32
    ) + jnp.einsum("erf,edf->erd", up_cot, w_up, preferred_element_type=jnp.float32)
    partial_value = lax.optimization_barrier(partial_value.astype(jnp.bfloat16)).astype(jnp.float32)
    share = lax.psum_scatter(
        partial_value.astype(jnp.bfloat16), "tp", scatter_dimension=2, tiled=True
    )
    channels = rec_input.shape[1]
    head_width = gate_a_w.shape[1]
    heads_here = channels // head_width
    first_head = lax.axis_index("tp") * heads_here
    decay_map = lax.dynamic_slice_in_dim(gate_a_w, first_head, heads_here, 0)
    input_map = lax.dynamic_slice_in_dim(gate_i_w, first_head, heads_here, 0)
    rates = lax.dynamic_slice_in_dim(decay_param, lax.axis_index("tp") * channels, channels, 0)
    rgate = jax.nn.sigmoid(head_product(rec_input, decay_map, False))
    igate = jax.nn.sigmoid(head_product(rec_input, input_map, False))
    rate_scale = decay_factor * jax.nn.softplus(-rates)
    log_decay = -rate_scale[None, :] * rgate + jnp.repeat(extra_decay.T, head_width, axis=1)
    decay = jnp.exp(log_decay)
    scale = jnp.sqrt(-jnp.expm1(2.0 * log_decay))
    values_in = rec_input.astype(jnp.float32)
    state = decay * prev_state + scale * igate * values_in
    gate_act, _ = gelu_pair(gate_input.astype(jnp.float32))
    rec_output = (state * gate_act).astype(jnp.bfloat16)
    share, grad_gate, grad_up, grad_down, log_decay, rgate, igate, rec_output = (
        lax.optimization_barrier(
            (share, grad_gate, grad_up, grad_down, log_decay, rgate, igate, rec_output)
        )
    )
    col_count = share.shape[-1]
    outgoing = jnp.swapaxes(share.reshape(local_experts, sources, capacity, col_count), 0, 1)
    outgoing = outgoing.reshape(sources, local_experts * capacity, col_count)
    returned = exchange([outgoing], [True], "sp", 2)[0].reshape(buffer_rows, col_count)
    slot_sum = lax.dot_general(
        pick, returned, (((0,), (0,)), ((), ())), preferred_element_type=jnp.float32
    )
    own_cot = lax.dynamic_slice_in_dim(out_cot, lax.axis_index("tp") * col_count, col_count, 1)
    part_cot = (own_cot.astype(jnp.float32) + slot_sum).astype(jnp.bfloat16)
    layer_cot = lax.all_gather(part_cot, "tp", axis=1, tiled=True)
    mix_cot = jnp.dot(layer_cot, out_proj, preferred_element_type=jnp.float32)
    decay = jnp.exp(log_decay)
    scale = jnp.sqrt(-jnp.expm1(2.0 * log_decay))
    values_in = rec_input.astype(jnp.float32)
    state = decay * prev_state + scale * igate * values_in
    gate_act, gate_slope = gelu_pair(gate_input.astype(jnp.float32))
    out_term = lax.dot_general(
        layer_cot, rec_output, (((0,), (0,)), ((), ())), preferred_element_type=jnp.float32
    ).astype(jnp.bfloat16)
    link = jnp.concatenate([decay[1:], jnp.ones((1, channels), jnp.float32)], axis=0)
    products, local_cot = reverse_scan(link, mix_cot * gate_act)
    edge = jnp.stack([decay[0] * products[0], decay[0] * local_cot[0]])
    edge = jnp.concatenate([edge, jnp.zeros((6, channels), jnp.float32)], axis=0)
    out_blocks = out_term.reshape(sources, width // sources, channels)
    gathered, out_terms = exchange([edge, out_blocks], [False, True], "sp", 3)
    grad_out_proj = jnp.sum(out_terms.astype(jnp.float32), axis=0)
    carried = carried_in(gathered, "sp")
    state_cot = local_cot + products * carried[None, :]
    gate_input_grad = (mix_cot * state * gate_slope).astype(jnp.bfloat16)
    log_cot = state_cot * (decay * prev_state - decay * decay / scale * igate * values_in)
    a_pre_cot = (log_cot * -rate_scale[None, :] * rgate * (1.0 - rgate)).astype(jnp.bfloat16)
    i_pre_cot = (state_cot * scale * values_in * igate * (1.0 - igate)).astype(jnp.bfloat16)
    rec_input_grad = (
        state_cot * scale * igate
        + head_product(a_pre_cot, decay_map, True)
        + head_product(i_pre_cot, input_map, True)
    ).astype(jnp.bfloat16)
    return (grad_gate, grad_up, grad_down, grad_out_proj, rec_input_grad, gate_input_grad)


def solution(mesh):
    in_specs = (
        P("sp", None),
        P("sp", None),
        P("sp", None),
        P("sp", None),
        P("sp", None, "tp"),
        P("sp", None, "tp"),
        P("sp", "tp", None),
        P(None, "tp"),
        P("sp", "tp"),
        P("sp", "tp"),
        P("sp", "tp"),
        P(),
        P("tp", "sp"),
        P(),
        P(),
    )
    out_specs = (
        P("sp", None, "tp"),
        P("sp", None, "tp"),
        P("sp", "tp", None),
        P("sp", "tp"),
        P("sp", "tp"),
        P("sp", "tp"),
    )
    return jax.shard_map(
        per_device, mesh=mesh, in_specs=in_specs, out_specs=out_specs, check_vma=False
    )
```
